512 devices in a mesh: fs: 16 (over y, x), tp: 32 (over z, core).
Axes of the slice: x: 4, y: 4, z: 16, core: 2. Of those that a mesh axis runs over, the one named last changes fastest.
Arguments:
- saved_input: bfloat16 [16384, 4096], P('fs', 'tp'), may hold values from -6 to 6
- query_cot: bfloat16 [16384, 4096], P('fs', 'tp'), may hold values from -6 to 6
- key_cot: bfloat16 [16384, 4096], P('fs', 'tp'), may hold values from -6 to 6
- query_master: float32 [4096, 4096], P('fs', 'tp'), may hold values from -0.09375 to 0.09375
- key_master: float32 [4096, 4096], P('fs', 'tp'), may hold values from -0.09375 to 0.09375
- query_basis: bfloat16 [4096, 256], P('fs'), may hold values from -3 to 3
- key_basis: bfloat16 [4096, 256], P('fs'), may hold values from -3 to 3
- query_first: float32 [256, 4096], P('fs', 'tp'), may hold values from -240 to 240
- query_second: float32 [256, 4096], P('fs', 'tp'), may hold values from 1000 to 20000
- key_first: float32 [256, 4096], P('fs', 'tp'), may hold values from -240 to 240
- key_second: float32 [256, 4096], P('fs', 'tp'), may hold values from 1000 to 20000
Outputs:
- query_step: float32 [4096, 4096], P('fs', 'tp')
- query_weight: float32 [4096, 4096], P('fs', 'tp')
- query_copy: bfloat16 [4096, 4096], P(None, 'tp')
- query_first_new: float32 [256, 4096], P('fs', 'tp')
- query_second_new: float32 [256, 4096], P('fs', 'tp')
- key_step: float32 [4096, 4096], P('fs', 'tp')
- key_weight: float32 [4096, 4096], P('fs', 'tp')
- key_copy: bfloat16 [4096, 4096], P(None, 'tp')
- key_first_new: float32 [256, 4096], P('fs', 'tp')
- key_second_new: float32 [256, 4096], P('fs', 'tp')
The draws below stay inside these ranges and needn't reach their ends.
All inputs are finite; a program needn't handle non-finite values.
Results may differ from the reference program's by a relative error of at most 0.0065.
Values may be sent and summed in bfloat16 or wider, within the bound.
A program may use at most 64 MiB of HBM per device.

```python
import math
import jax
import jax.numpy as jnp
from jax import lax

D = 4096
HEADS = 32
HD = 128
RANK = 256
TOKENS = 16384


def basis_draw(key, salt):
    base = jax.random.fold_in(key, salt)
    entry_key, factor_key = jax.random.split(base)
    group = max(D // 64, 1)
    groups = D // group
    entries = jnp.clip(jax.random.normal(entry_key, (D, RANK), jnp.float32), -4.0, 4.0)
    factors = jnp.exp(jax.random.uniform(factor_key, (groups,), jnp.float32, -1.5, 1.5))
    row_scale = jnp.repeat(factors, group)
    values = entries * row_scale[:, None] * D ** (-0.5)
    return values.astype(jnp.bfloat16)


def draw_query_basis(key, part):
    return basis_draw(key, 101)


def draw_key_basis(key, part):
    return basis_draw(key, 202)


def block_scale(key, dims, pieces, low, largest):
    loudness, own = 1.0, jax.random.fold_in(key, 6)
    for position, blocks in pieces:
        steps = jnp.exp(jax.random.uniform(jax.random.fold_in(own, position), (blocks,), jnp.float32, low / len(pieces), largest / len(pieces)))
        loudness = loudness * jnp.repeat(steps, dims[position] // blocks).reshape([-1 if axis == position else 1 for axis in range(len(dims))])
    return loudness


def bell_draw(stream_key, shape, scale, most, cuts=(), kind=jnp.bfloat16):
    values = jax.random.normal(stream_key, shape, jnp.float32) * scale
    if len(cuts) > 0:
        values = block_scale(stream_key, shape, cuts, -0.22, 0.18) * values
    return jnp.clip(values, min=-most, max=most).astype(kind)


def setup_inputs(seed: int = 0) -> dict:
    seeds = jax.random.split(jax.random.key(seed), 12)
    saved_input = bell_draw(seeds[0], (TOKENS, D), 1.0, 6.0, ((0, 16), (1, 32)))
    query_cot = bell_draw(seeds[1], (TOKENS, HEADS * HD), 1.0, 6.0, ((0, 16), (1, 32)))
    key_cot = bell_draw(seeds[2], (TOKENS, HEADS * HD), 1.0, 6.0, ((0, 16), (1, 32)))
    query_master = bell_draw(seeds[3], (D, HEADS * HD), D ** -0.5, 0.09375, ((0, 16), (1, 32)), jnp.float32)
    key_master = bell_draw(seeds[4], (D, HEADS * HD), D ** -0.5, 0.09375, ((0, 16), (1, 32)), jnp.float32)
    query_basis = draw_query_basis(jax.random.fold_in(seeds[11], 71), 0)
    key_basis = draw_key_basis(jax.random.fold_in(seeds[11], 71), 0)
    query_first = bell_draw(seeds[7], (RANK, HEADS * HD), 40.0, 240.0, ((0, 16), (1, 32)), jnp.float32)
    query_second = jnp.clip(jnp.exp(math.log(20000.0) - 2.9957323 * jax.random.uniform(seeds[8], (RANK, HEADS * HD), jnp.float32) ** block_scale(seeds[8], (RANK, HEADS * HD), ((0, 16), (1, 32)), -0.2, 0.2)), 1000.0, 20000.0)
    key_first = bell_draw(seeds[9], (RANK, HEADS * HD), 40.0, 240.0, ((0, 16), (1, 32)), jnp.float32)
    key_second = jnp.clip(jnp.exp(math.log(20000.0) - 2.9957323 * jax.random.uniform(seeds[10], (RANK, HEADS * HD), jnp.float32) ** block_scale(seeds[10], (RANK, HEADS * HD), ((0, 16), (1, 32)), -0.2, 0.2)), 1000.0, 20000.0)
    return {"saved_input": saved_input, "query_cot": query_cot, "key_cot": key_cot, "query_master": query_master, "key_master": key_master, "query_basis": query_basis, "key_basis": key_basis, "query_first": query_first, "query_second": query_second, "key_first": key_first, "key_second": key_second}


moment_decay = 0.8
square_decay = 0.9
square_floor = 1.0
norm_floor = 0.01
step_rate = 0.01

def update_one(saved_input, cotangent, master, basis, first, second):
    grad = jnp.dot(saved_input.T, cotangent, preferred_element_type=jnp.float32)
    low = jnp.dot(basis.astype(jnp.float32).T, grad, precision=lax.Precision.HIGHEST)
    first_new = moment_decay * first + (1.0 - moment_decay) * low
    second_new = square_decay * second + (1.0 - square_decay) * low * low
    ratio = (first_new / jnp.sqrt(second_new + square_floor)).astype(jnp.bfloat16)
    update = jnp.dot(basis, ratio, preferred_element_type=jnp.float32)
    by_head = update.reshape(D, HEADS, HD)
    head_mean = lax.optimization_barrier(jnp.mean(by_head * by_head, axis=(0, 2)))
    head_scale = 1.0 / jnp.sqrt(head_mean + norm_floor)
    step = (by_head * head_scale[None, :, None]).reshape(D, HEADS * HD)
    weight = master - step_rate * step
    return (step, weight, weight.astype(jnp.bfloat16), first_new, second_new)

def reference(saved_input, query_cot, key_cot, query_master, key_master, query_basis, key_basis, query_first, query_second, key_first, key_second):
    query_out = update_one(saved_input, query_cot, query_master, query_basis, query_first, query_second)
    key_out = update_one(saved_input, key_cot, key_master, key_basis, key_first, key_second)
    return (query_out[0], query_out[1], query_out[2], query_out[3], query_out[4], key_out[0], key_out[1], key_out[2], key_out[3], key_out[4])
```

```python
import contextlib
import functools

import jax
import jax.numpy as jnp
from jax import lax
from jax.experimental import pallas as pl
from jax.experimental.pallas import tpu as pltpu
from jax.sharding import PartitionSpec as P

HD = 128
SIDE = 4

moment_decay = 0.8
square_decay = 0.9
square_floor = 1.0
norm_floor = 0.01
step_rate = 0.01

BF = jnp.bfloat16
F32 = jnp.float32
MESH = pl.DeviceIdType.MESH
SCOPES = False


def scope(name):
    return jax.named_scope(name) if SCOPES else contextlib.nullcontext()


def wrap(offset):
    return (offset + 1) % SIDE - 1


ARRIVALS = [(-1, 0, None), (1, 0, None), (2, 0, 0), (2, 0, 1)]
for near in (-1, 1):
    ARRIVALS += [(0, near, None), (-1, near, None), (1, near, None), (2, near, 0), (2, near, 1)]
for u in (0, -1, 1, 2):
    ARRIVALS += [(u, 2, 0), (u, 2, 1)]
SLOT = {
    (kind, *key): kind * len(ARRIVALS) + place
    for kind in range(2)
    for place, key in enumerate(ARRIVALS)
}


def forwards(u, v, part):
    onward = []
    if v == 0:
        if u == -1:
            onward.append((0, 0, 1))
        if u == 1:
            onward.append((1, 0, -1))
        onward += [(part, 1, 1), (part, 1, -1)]
    elif v == -1 and part != 1:
        onward.append((0, 1, 1))
    elif v == 1 and part != 0:
        onward.append((1, 1, -1))
    return onward


class Gather:
    def __init__(self, piece, send_sem, recv_sem, x, y, t):
        self.piece, self.send_sem, self.recv_sem = piece, send_sem, recv_sem
        self.x, self.y, self.t = x, y, t
        self.copies = []

    def owner(self, kind, u, v):
        dx, dy = (u, v) if kind == 0 else (v, u)
        return lax.rem(self.y + dy + SIDE, SIDE) * SIDE + lax.rem(self.x + dx + SIDE, SIDE)

    def copy(self, kind, u, v, part, axis, direction):
        step = (direction, 0) if axis == 0 else (0, direction)
        slot = SLOT[kind, wrap(u - step[0]), wrap(v - step[1]), part]
        ref = self.piece(kind, self.owner(kind, u, v), part)
        return pltpu.make_async_remote_copy(
            src_ref=ref,
            dst_ref=ref,
            send_sem=self.send_sem.at[slot],
            recv_sem=self.recv_sem.at[slot],
            device_id=(self.owner(kind, *step), self.t),
            device_id_type=MESH,
        )

    def send(self, kind, u, v, part, axis, direction):
        copy = self.copy(kind, u, v, part, axis, direction)
        copy.start()
        self.copies.append(copy)

    def start(self):
        for axis in range(2):
            for kind in range(2):
                for direction in (1, -1):
                    self.send(kind, 0, 0, None, axis, direction)

    def wait(self, kind, u, v, part):
        ref = self.piece(kind, self.owner(kind, u, v), part)
        slot = SLOT[kind, u, v, part]
        pltpu.make_async_remote_copy(
            src_ref=ref,
            dst_ref=ref,
            send_sem=self.send_sem.at[slot],
            recv_sem=self.recv_sem.at[slot],
            device_id=(self.owner(kind, 1, 0), self.t),
            device_id_type=MESH,
        ).wait_recv()

    def take(self, *keys):
        for u, v, part in keys:
            for kind in range(2):
                self.wait(kind, u, v, part)
                for onward, axis, direction in forwards(u, v, part):
                    self.send(kind, u, v, onward, axis, direction)


STAGES = [
    [(-1, 0, None), (1, 0, None)],
    [(0, -1, None), (0, 1, None)],
    [(2, 0, 0), (2, 0, 1)],
    [(-1, -1, None), (-1, 1, None), (1, -1, None), (1, 1, None)],
    [(2, -1, 0), (2, 1, 1), (2, -1, 1), (2, 1, 0)],
    [(0, 2, 0), (0, 2, 1)],
    [(u, 2, part) for u in (-1, 1, 2) for part in range(2)],
]


def exchange_kernel(
    fs,
    tp,
    x_ref,
    qc_ref,
    kc_ref,
    qm_ref,
    km_ref,
    qb_ref,
    kb_ref,
    qf_ref,
    qs_ref,
    kf_ref,
    ks_ref,
    qfn_ref,
    qsn_ref,
    kfn_ref,
    ksn_ref,
    scale_ref,
    gathered,
    update_ref,
    own_ref,
    ratio_ref,
    basis,
    x_all,
    acc,
    low,
    proj,
    proj_send,
    proj_recv,
    b_send,
    b_recv,
    m_send,
    m_recv,
    x_send,
    x_recv,
    xd_send,
    xd_recv,
    z_send,
    z_recv,
    zd_send,
    zd_recv,
    d_send,
    d_recv,
    rs_send,
    rs_recv,
    ag_send,
    ag_recv,
):
    f = lax.axis_index("fs")
    t = lax.axis_index("tp")
    z, c = t // 2, t % 2
    x, y = f % SIDE, f // SIDE
    partner = (f, t + 1 - 2 * c)
    depth = tp // 2
    rows, rank = qb_ref.shape
    width = qc_ref.shape[1]
    tokens, columns = x_ref.shape
    part_rows = rank // fs
    chunk = tokens // depth
    half = rows // 2

    def at(start, size):
        return pl.ds(pl.multiple_of(start, size), size)

    def remote(src, dst, send, recv, target):
        return pltpu.make_async_remote_copy(
            src_ref=src,
            dst_ref=dst,
            send_sem=send,
            recv_sem=recv,
            device_id=target,
            device_id_type=MESH,
        )

    def along(offset):
        return lax.rem(z + offset + depth, depth)

    sent = []

    def go(copy):
        copy.start()
        sent.append(copy)

    own_rows = at(f * rows, rows)
    with scope("barrier"):
        barrier = pltpu.get_barrier_semaphore()

        def greet(target):
            pl.semaphore_signal(barrier, inc=1, device_id=target, device_id_type=MESH)

        for d in range(1, depth):
            greet((f, along(d) * 2 + c))
        for m in range(1, fs):
            greet((f ^ m, t))
        greet(partner)
        for j, (own_basis, master) in enumerate(((qb_ref, qm_ref), (kb_ref, km_ref))):
            basis[j, own_rows, :] = own_basis[...]
            gathered[j, own_rows, :] = master[...].astype(BF)
        x_all[c, z] = x_ref[at(z * chunk, chunk), :]
        pl.semaphore_wait(barrier, fs - 1 + depth)

    def basis_piece(kind, owner, part):
        start, size = owner * rows + kind * half, half
        if part is not None:
            start, size = start + part * (half // 2), half // 2
        return basis.at[c, at(start, size)]

    def master_piece(kind, owner, part):
        start, size = owner * rows, rows
        if part is not None:
            start, size = start + part * half, half
        return gathered.at[kind, at(start, size)]

    bases = Gather(basis_piece, b_send, b_recv, x, y, t)
    masters = Gather(master_piece, m_send, m_recv, x, y, t)

    bases.start()

    def x_copy(e):
        return remote(
            x_ref.at[at(along(e) * chunk, chunk)],
            x_all.at[c, z],
            x_send.at[e % depth],
            x_recv.at[-e % depth],
            (f, along(e) * 2 + c),
        )

    far = depth // 2
    offsets = [far] + [s * e for e in range(far - 1, 0, -1) for s in (1, -1)]
    for e in offsets:
        go(x_copy(e))
    go(
        remote(
            x_ref.at[at(z * chunk, chunk)], x_all.at[c, z], xd_send.at[0], xd_recv.at[0], partner
        )
    )

    def x_wait(e):
        piece = x_all.at[c, along(e)]
        remote(
            piece, piece, x_send.at[e % depth], x_recv.at[e % depth], (f, along(e) * 2 + c)
        ).wait_recv()

    def x_take(e):
        x_wait(e)
        piece = x_all.at[c, along(e)]
        go(remote(piece, piece, xd_send.at[e % depth], xd_recv.at[e % depth], partner))

    def x_partner(e):
        piece = x_all.at[1 - c, along(e)]
        remote(
            piece, piece, xd_send.at[e % depth], xd_recv.at[e % depth], partner
        ).wait_recv()

    with scope("basis"):
        acc[...] = jnp.zeros_like(acc)
        for stage in STAGES[:5]:
            bases.take(*stage)
    masters.start()
    with scope("x_wait"):
        for e in offsets:
            x_take(e)
    with scope("x_partner"):
        for e in [0] + offsets:
            x_partner(e)

    def project(u, v):
        owner = lax.rem(y + v + SIDE, SIDE) * SIDE + lax.rem(x + u + SIDE, SIDE)
        per = depth * 2 * columns // (fs * rows) * rows // columns
        for i in range(per // 2):
            group = owner * (per // 2) + i
            both = jnp.concatenate([x_all[0, group], x_all[1, group]], axis=1)
            place = at(owner * rows + i * 2 * columns, 2 * columns)
            acc[...] += jnp.dot(both, basis[c, place, :], preferred_element_type=F32)

    with scope("project"):
        for u in (0, -1, 1):
            for v in (0, -1, 1):
                project(u, v)
    with scope("basis_end"):
        for stage in STAGES[5:]:
            bases.take(*stage)
    with scope("project_end"):
        for u in (0, -1, 1, 2):
            project(u, 2)
        for v in (0, -1, 1):
            project(2, v)
        low[c, at(z * chunk, chunk), :] = acc[...].astype(BF)

    def low_rows(e, part=None):
        start, size = along(e) * chunk, chunk
        if part is not None:
            start, size = start + part * (chunk // 2), chunk // 2
        return at(start, size)

    def z_slot(e, part=None):
        return depth if part == 1 else e % depth

    def z_go(e, hop, part=None):
        piece = low.at[c, low_rows(e, part)]
        slot = z_slot(e - hop, part)
        go(
            remote(
                piece, piece, z_send.at[slot], z_recv.at[slot], (f, along(hop) * 2 + c)
            )
        )

    def z_wait(e, part=None):
        piece = low.at[c, low_rows(e, part)]
        slot = z_slot(e, part)
        remote(piece, piece, z_send.at[slot], z_recv.at[slot], partner).wait_recv()

    def z_partner(e, j):
        piece = low.at[j, low_rows(e)]
        return remote(piece, piece, zd_send.at[e % depth], zd_recv.at[e % depth], partner)

    def spread(e, sign):
        reach = abs(e)
        if reach + 2 < far:
            z_go(e, 2 * sign)
        elif reach + 2 == far:
            z_go(e, 2 * sign, 0 if sign > 0 else 1)
        z_go(e, sign)

    def z_take(e):
        z_wait(e)
        if abs(e) % 2 == 0 and abs(e) < far:
            spread(e, 1 if e < 0 else -1)
        go(z_partner(e, c))

    def share(m):
        piece = basis.at[c, at((f ^ m) * rows, rows)]
        return remote(piece, piece, d_send.at[m], d_recv.at[m], partner)

    with scope("z_start"):
        for sign in (1, -1):
            spread(0, sign)
        go(z_partner(0, c))
        for m in range(1, fs):
            go(share(m))

    with scope("z_gather"):
        masters.take(*STAGES[0])
        masters.take(*STAGES[1])
        reach = 2
        stage = 2
        while reach < far:
            for e in (-reach, reach, 1 - reach, reach - 1):
                z_take(e)
            if stage < 5:
                masters.take(*STAGES[stage])
                stage += 1
            reach += 2
        for e in (1 - far, far - 1):
            z_take(e)
        z_wait(far, 0)
        z_wait(far, 1)
        go(z_partner(far, c))
    with scope("z_partner"):
        for e in [0] + offsets:
            z_partner(e, 1 - c).wait_recv()

    with scope("low"):
        for j, cot in enumerate((qc_ref, kc_ref)):
            product = lax.dot_general(
                low[j], cot[...], (((0,), (0,)), ((), ())), preferred_element_type=F32
            )
            proj[j] = product
            proj_send[j] = product.astype(BF)
    with scope("reduce"):
        for m in range(fs - 1, 0, -1):
            go(
                remote(
                    proj_send.at[:, at((f ^ m) * part_rows, part_rows)],
                    proj_recv.at[m],
                    rs_send.at[m],
                    rs_recv.at[m],
                    (f ^ m, t),
                )
            )
        while stage < len(STAGES):
            masters.take(*STAGES[stage])
            stage += 1
        for m in range(1, fs):
            remote(
                proj_recv.at[m], proj_recv.at[m], rs_send.at[m], rs_recv.at[m], (f ^ m, t)
            ).wait_recv()

    own = at(f * part_rows, part_rows)
    with scope("moments"):
        moments = ((qf_ref, qs_ref, qfn_ref, qsn_ref), (kf_ref, ks_ref, kfn_ref, ksn_ref))
        for j, (first, second, first_out, second_out) in enumerate(moments):
            summed = proj[j, own, :]
            for m in range(1, fs):
                summed = summed + proj_recv[m, j].astype(F32)
            first_new = moment_decay * first[...] + (1.0 - moment_decay) * summed
            second_new = square_decay * second[...] + (1.0 - square_decay) * summed * summed
            first_out[...] = first_new
            second_out[...] = second_new
            ratio_ref[j, own, :] = (first_new / jnp.sqrt(second_new + square_floor)).astype(BF)

    def ratio_copy(m, owner):
        piece = ratio_ref.at[:, at(owner * part_rows, part_rows)]
        return remote(piece, piece, ag_send.at[m], ag_recv.at[m], (f ^ m, t))

    with scope("ratio"):
        for m in range(fs - 1, 0, -1):
            go(ratio_copy(m, f))
        for m in range(1, fs):
            piece = basis.at[1 - c, at((f ^ m) * rows, rows)]
            remote(piece, piece, d_send.at[m], d_recv.at[m], partner).wait_recv()
        for m in range(1, fs):
            ratio_copy(m, f ^ m).wait_recv()

    with scope("update"):
        high = min(fs * rows, 512)
        for j in range(2):

            def add(i, total, j=j):
                place = at(i * high, high)
                update = jnp.dot(
                    basis[j, place, :], ratio_ref[j], preferred_element_type=F32
                )
                update_ref[j, place, :] = update
                return total + jnp.sum((update * update).reshape(high // 8, 8, width), axis=0)

            sums = lax.fori_loop(0, fs * rows // high, add, jnp.zeros((8, width), F32))
            sums = jnp.sum(sums, axis=0, keepdims=True)
            for h in range(width // HD):
                head = slice(h * HD, (h + 1) * HD)
                total = jnp.sum(sums[:, head], axis=1, keepdims=True)
                scale = 1.0 / jnp.sqrt(total / (fs * rows * HD) + norm_floor)
                scale_ref[j, :, head] = jnp.broadcast_to(scale, (8, HD))
            own_ref[j] = update_ref[j, own_rows, :]

    with scope("drain"):
        for copy in sent + bases.copies + masters.copies:
            copy.wait_send()


def final_kernel(scale_ref, update_ref, gathered_ref, own_ref, qm_ref, km_ref, *refs):
    moments, outs, moments_out = refs[:4], refs[4:10], refs[10:]
    for j, master in enumerate((qm_ref, km_ref)):
        scale = scale_ref[j, 0:1, :]
        step_out, weight_out, copy_out = outs[3 * j : 3 * j + 3]
        step = own_ref[j] * scale
        step_out[...] = step
        weight_out[...] = master[...] - step_rate * step
        step = update_ref[j] * scale
        copy_out[...] = (gathered_ref[j].astype(F32) - step_rate * step).astype(BF)

    @pl.when(pl.program_id(0) == 0)
    def _():
        for source, target in zip(moments, moments_out):
            target[...] = source[...]


def body(fs, tp, *args):
    saved_input, query_cot, _, query_master, key_master, query_basis, key_basis = args[:7]
    rows, rank = query_basis.shape
    tokens, columns = saved_input.shape
    width = query_cot.shape[1]
    part = rank // fs
    depth = tp // 2
    count = fs * rows
    chunk = tokens // depth
    vmem = pl.BlockSpec(memory_space=pltpu.VMEM)
    dma = pltpu.SemaphoreType.DMA
    moment = jax.ShapeDtypeStruct((part, width), F32)
    pairs = []
    slots = (2 * len(ARRIVALS), 2 * len(ARRIVALS), depth, depth, depth + 1, depth, fs, fs, fs)
    for slot in slots:
        pairs += [dma((slot,)), dma((slot,))]
    results = pl.pallas_call(
        functools.partial(exchange_kernel, fs, tp),
        name="exchange",
        out_shape=(
            moment,
            moment,
            moment,
            moment,
            jax.ShapeDtypeStruct((2, 8, width), F32),
            jax.ShapeDtypeStruct((2, count, width), BF),
            jax.ShapeDtypeStruct((2, count, width), F32),
            jax.ShapeDtypeStruct((2, rows, width), F32),
        ),
        in_specs=[vmem] * 11,
        out_specs=(vmem,) * 8,
        scratch_shapes=[
            pltpu.VMEM((2, rank, width), BF),
            pltpu.VMEM((2, count, rank), BF),
            pltpu.VMEM((2, depth, chunk, columns), BF),
            pltpu.VMEM((chunk, rank), F32),
            pltpu.VMEM((2, tokens, rank), BF),
            pltpu.VMEM((2, rank, width), F32),
            pltpu.VMEM((2, rank, width), BF),
            pltpu.VMEM((fs, 2, part, width), BF),
            *pairs,
        ],
        compiler_params=pltpu.CompilerParams(
            collective_id=0, has_side_effects=True, vmem_limit_bytes=24 * 1024 * 1024
        ),
    )(*args)
    moments, (scale, gathered, update, own) = results[:4], results[4:]

    steps = min(8, rows // 16)
    own_tile, tile = rows // steps, count // steps

    def row(i):
        return (i, 0)

    def pair(i):
        return (0, i, 0)

    def whole(i):
        return (0, 0, 0)

    own_spec = pl.BlockSpec((own_tile, width), row)
    full_spec = pl.BlockSpec((tile, width), row)
    moment_spec = pl.BlockSpec((part, width), lambda i: (0, 0))
    big = jax.ShapeDtypeStruct((rows, width), F32)
    copied = jax.ShapeDtypeStruct((count, width), BF)
    outs = pl.pallas_call(
        final_kernel,
        name="final",
        out_shape=(big, big, copied) * 2 + (moment,) * 4,
        grid=(steps,),
        in_specs=[
            pl.BlockSpec((2, 8, width), whole),
            pl.BlockSpec((2, tile, width), pair),
            pl.BlockSpec((2, tile, width), pair),
            pl.BlockSpec((2, own_tile, width), pair),
            own_spec,
            own_spec,
        ]
        + [moment_spec] * 4,
        out_specs=(own_spec, own_spec, full_spec) * 2 + (moment_spec,) * 4,
        compiler_params=pltpu.CompilerParams(vmem_limit_bytes=24 * 1024 * 1024),
    )(scale, update, gathered, own, query_master, key_master, *moments)
    return (*outs[:3], *outs[6:8], *outs[3:6], *outs[8:])


def solution(mesh):
    split, tall, wide = P("fs", "tp"), P("fs", None), P(None, "tp")
    outs = (split, split, wide, split, split)
    return jax.shard_map(
        functools.partial(body, mesh.shape["fs"], mesh.shape["tp"]),
        mesh=mesh,
        in_specs=(split,) * 5 + (tall, tall) + (split,) * 4,
        out_specs=outs + outs,
        check_vma=False,
    )
```
